256 devices in a mesh: ep: 64 (over z, y, core), tp: 4 (over x).
Axes of the slice: x: 4, y: 4, z: 8, core: 2. Of those that a mesh axis runs over, the one named last changes fastest.
Arguments:
- tokens: bfloat16 [16384, 2048], P('ep'), may hold values from -6 to 6
- expert_ids: int32 [16384, 2], P('ep'), may hold values from 0 to 63, all different within a row; in each aligned block of 256 rows (0 to 255, 256 to 511, ...) at most 24 rows name the same one
- route_weight: float32 [16384, 2], P('ep'), may hold values from 0.1 to 1
- norm_gain: float32 [2048], replicated, may hold values from 0.1 to 1.9
- expert_gate: bfloat16 [64, 2048, 2048], P('ep', None, 'tp'), may hold values from -4 to 4
- expert_up: bfloat16 [64, 2048, 2048], P('ep', None, 'tp'), may hold values from -4 to 4
- expert_down: bfloat16 [64, 2048, 2048], P('ep', 'tp'), may hold values from -0.03125 to 0.03125
Outputs:
- combined: bfloat16 [16384, 2048], P('ep', 'tp')
The draws below stay inside these ranges and needn't reach their ends.
Inputs may be any that keep to these rules, and one draw needn't show every extreme that they name: `expert_ids`: each row names 2 different experts. In each aligned block of 256 rows (the rows of one index of ep) no expert is named by more than 24 rows, and in some block one expert is named by exactly 24 rows.
All inputs are finite; a program needn't handle non-finite values.
Results may differ from the reference program's by a relative error of at most 0.012.
Values may be sent and summed in bfloat16 or wider, within the bound.
No kernel may reach another device: no remote copies, remote signals or barrier semaphores. Data moves between devices by JAX's collectives and lax.ppermute only.
A program may use at most 128 MiB of HBM per device.

```python
import math
import jax
import jax.numpy as jnp
import numpy as np
from jax import lax

D = 2048
FF = 2048
TOP_K = 2
TOK_GROUP = 256
EXPERTS = 64
TOKENS = 16384
CAP = 24
N_EP = 64
N_TP = 4


def draw_expert_gate(key, part):
    spread = 3.0
    normal_draw = jax.random.truncated_normal(jax.random.fold_in(key, 11), -4.0, 4.0, (EXPERTS, D, FF), jnp.float32)
    return (normal_draw * (spread / math.sqrt(D))).astype(jnp.bfloat16)


def draw_expert_up(key, part):
    spread = 3.0
    normal_draw = jax.random.truncated_normal(jax.random.fold_in(key, 23), -4.0, 4.0, (EXPERTS, D, FF), jnp.float32)
    return (normal_draw * (spread / math.sqrt(D))).astype(jnp.bfloat16)


def shard_levels(rng, shape, shards, least, largest):
    gain = 1.0
    for dim, blocks in shards:
        draws = jax.random.uniform(jax.random.fold_in(jax.random.fold_in(rng, 6), dim), (blocks,), jnp.float32, least / len(shards), largest / len(shards))
        gain = gain * jnp.repeat(jnp.exp(draws), shape[dim] // blocks).reshape((-1,) + (1,) * (len(shape) - 1 - dim))
    return gain


def routed_block(own_key, own, number, rows, amount, top, limit, skew):
    order = jax.random.permutation(own_key, amount)
    heavy_load, ordinary = portions_of(amount, rows * top, limit, skew, True), portions_of(amount, rows * top, limit, skew, False)
    places = jnp.arange(amount)

    def named(tallies, rotation):
        used = int((tallies > 0).sum())
        fixed = max(1, used // 4)
        shifted = fixed + (places - fixed + rotation * (used - fixed)) % max(1, amount - fixed)
        return jnp.zeros((amount,), jnp.int32).at[order[jnp.where(places < fixed, places, shifted)]].set(jnp.asarray(tallies, jnp.int32))

    tallies = jnp.where(number % 4 == 0, named(heavy_load, number // 4), named(ordinary, number - number // 4 - 1))
    mixed = jax.random.permutation(jax.random.fold_in(own, 3), amount)
    giver, sink = mixed[0:amount // 2 * 2:2], mixed[1:amount // 2 * 2:2]
    room = jnp.minimum(tallies[giver] - 1, limit - tallies[sink]) // 2
    room = jnp.where((giver == order[0]) | (sink == order[0]) | (tallies[sink] == 0), 0, jnp.maximum(room, 0))
    shifted = jax.random.randint(jax.random.fold_in(own, 4), (amount // 2,), 0, 1 << 20) % (room + 1)
    tallies = tallies.at[giver].add(-shifted).at[sink].add(shifted)
    labels = jnp.searchsorted(jnp.cumsum(tallies), jnp.arange(rows * top), side="right").astype(jnp.int32)
    table = labels.reshape(top, rows).T
    table = table[jax.random.permutation(jax.random.fold_in(own, 1), rows)]
    rotation = jax.random.randint(jax.random.fold_in(own, 2), (rows, 1), 0, top)
    return jnp.take_along_axis(table, (jnp.arange(top)[None, :] + rotation) % top, axis=1)


def portions_of(count, total, most, skew, full):
    loads = [(1 << 20) // math.isqrt(grade ** skew) + 1 for grade in range(1, count + 1)]
    largest = most if full else min(most, max(-(-total // count), total * loads[0] // sum(loads)))
    least = 1 if total - largest >= count - 1 else 0
    counts, surplus = [largest] + [least] * (count - 1), total - largest - least * (count - 1)
    while surplus > 0:
        candidates = [i for i in range(1, count) if counts[i] < largest] or [i for i in range(1, count) if counts[i] < most]
        mass, remaining = sum([loads[i] for i in candidates]), surplus
        for i in candidates:
            more = min(most - counts[i], max(1, remaining * loads[i] // mass), surplus)
            counts[i] = counts[i] + more
            surplus = surplus - more
    return np.array(counts)


def bell_draw(key, shape, scale, most, pieces=(), kind=jnp.bfloat16):
    result = jax.random.normal(key, shape, jnp.float32) * scale
    if len(pieces) > 0:
        result = shard_levels(key, shape, pieces, -0.22, 0.18) * result
    return jnp.clip(result, min=-most, max=most).astype(kind)


def setup_inputs(seed: int = 0) -> dict:
    key_list = jax.random.split(jax.random.key(seed), 8)
    tokens = bell_draw(key_list[0], (TOKENS, D), 1.0, 6.0, ((0, 64),))
    expert_ids_keys = jax.random.split(jax.random.fold_in(key_list[1], 1), TOKENS // TOK_GROUP)
    expert_ids_turns = jax.random.permutation(jax.random.fold_in(key_list[1], 3), TOKENS // TOK_GROUP)
    expert_ids = jax.vmap(lambda own, number: routed_block(jax.random.fold_in(key_list[1], 2), own, number, TOK_GROUP, EXPERTS, TOP_K, CAP, 1))(expert_ids_keys, expert_ids_turns).reshape((TOKENS, TOP_K))
    route_weight = jnp.clip(0.1 + 0.9 * jax.random.uniform(key_list[2], (TOKENS, TOP_K), jnp.float32) ** shard_levels(key_list[2], (TOKENS, TOP_K), ((0, 64),), -0.2, 0.2), 0.1, 1.0)
    norm_gain = jnp.clip(1.0 + 0.18 * jax.random.normal(key_list[3], (D,), jnp.float32), 0.1, 1.9)
    expert_gate = draw_expert_gate(jax.random.fold_in(key_list[7], 71), 0)
    expert_up = draw_expert_up(jax.random.fold_in(key_list[7], 71), 0)
    expert_down = bell_draw(key_list[6], (EXPERTS, FF, D), (16 * FF) ** -0.5, 0.03125, ((0, 64), (1, 4)))
    return dict(tokens=tokens, expert_ids=expert_ids, route_weight=route_weight, norm_gain=norm_gain, expert_gate=expert_gate, expert_up=expert_up, expert_down=expert_down)


NORM_EPS = 1e-06
CLAMP_LIMIT = 7.0
SWISH_SCALE = 1.702

def normalize(tokens, norm_gain):
    values = tokens.astype(jnp.float32)
    scaled = values * lax.rsqrt(lax.optimization_barrier(jnp.mean(values * values, axis=-1, keepdims=True)) + NORM_EPS)
    return (scaled * norm_gain).astype(jnp.bfloat16)

def activate(gate_sum, up_sum):
    gate_cut = jnp.minimum(gate_sum, CLAMP_LIMIT)
    up_cut = jnp.clip(up_sum, -CLAMP_LIMIT, CLAMP_LIMIT)
    return ((up_cut + 1.0) * gate_cut * jax.nn.sigmoid(SWISH_SCALE * gate_cut)).astype(jnp.bfloat16)

def reference(tokens, expert_ids, route_weight, norm_gain, expert_gate, expert_up, expert_down):
    normed = normalize(tokens, norm_gain)
    flat_ids = expert_ids.reshape(N_EP, TOK_GROUP * TOP_K)
    onehot = (flat_ids[:, :, None] == jnp.arange(EXPERTS, dtype=jnp.int32)[None, None, :]).astype(jnp.int32)
    slot_index = lax.optimization_barrier(jnp.sum(jnp.cumsum(onehot, axis=1) * onehot, axis=2)) - 1
    block_index = jnp.arange(N_EP, dtype=jnp.int32)[:, None]
    token_index = block_index * TOK_GROUP + jnp.arange(TOK_GROUP * TOP_K, dtype=jnp.int32)[None, :] // TOP_K
    position = (block_index * CAP + slot_index).astype(jnp.int32)
    row_table = jnp.full((EXPERTS, N_EP * CAP), TOKENS, jnp.int32).at[flat_ids, position].set(token_index.astype(jnp.int32))
    padded = jnp.concatenate([normed, jnp.zeros((1, D), jnp.bfloat16)], axis=0)
    quarter = FF // N_TP

    def one_expert(operands):
        rows_index, gate_w, up_w, down_w = operands
        picked = padded[rows_index]
        gate_sum = jnp.dot(picked, gate_w, preferred_element_type=jnp.float32)
        up_sum = jnp.dot(picked, up_w, preferred_element_type=jnp.float32)
        activated = activate(gate_sum, up_sum)
        total_sum = jnp.zeros((picked.shape[0], D), jnp.float32)
        for shard_number in range(N_TP):
            lower = shard_number * quarter
            partial_value = jnp.dot(activated[:, lower:lower + quarter], down_w[lower:lower + quarter], preferred_element_type=jnp.float32)
            rounded = lax.optimization_barrier(partial_value.astype(jnp.bfloat16))
            total_sum = total_sum + rounded.astype(jnp.float32)
        return total_sum.astype(jnp.bfloat16)
    outputs = lax.map(one_expert, (row_table, expert_gate, expert_up, expert_down))
    flat_out = outputs.reshape(EXPERTS * N_EP * CAP, D)
    out_index = (flat_ids * (N_EP * CAP) + position).reshape(-1)
    chosen = flat_out[out_index].reshape(TOKENS, TOP_K, D).astype(jnp.float32)
    combined = lax.optimization_barrier(jnp.sum(chosen * route_weight[:, :, None], axis=1))
    return combined.astype(jnp.bfloat16)
```

```python
import jax
import jax.numpy as jnp
from jax import lax
from jax.experimental import pallas as pl
from jax.experimental.pallas import tpu as pltpu
from jax.sharding import PartitionSpec as P


NORM_EPS = 1e-06
CLAMP_LIMIT = 7.0
SWISH_SCALE = 1.702
SLOTS = 8
VMEM_BYTES = 20 << 20
INTERPRET = False


def activate(gate_sum, up_sum):
    gate_cut = jnp.minimum(gate_sum, CLAMP_LIMIT)
    up_cut = jnp.clip(up_sum, -CLAMP_LIMIT, CLAMP_LIMIT)
    return ((up_cut + 1.0) * gate_cut * jax.nn.sigmoid(SWISH_SCALE * gate_cut)).astype(jnp.bfloat16)


def dot(a, b):
    return jnp.dot(a, b, preferred_element_type=jnp.float32)


def first_body(own, near_a, near_b, gate_w, up_w, gate_out, up_out):
    rows, quarter = own.shape
    step = rows // 2
    for top in range(0, rows, step):
        at = slice(top, top + step)
        for w, out in ((gate_w, gate_out), (up_w, up_out)):
            total = dot(own[at, :], w[:quarter, :])
            total = total + dot(near_a[at, :], w[quarter : 2 * quarter, :])
            out[at, :] = total + dot(near_b[at, :], w[2 * quarter :, :])


def last_body(gate_sum, up_sum, far_a, far_b, gate_w, up_w, down_far, down_near, *outs):
    across_a, across_b, for_a, for_b, kept = outs
    half, quarter = far_a.shape
    for part, (far, across) in enumerate(((far_a, across_a), (far_b, across_b))):
        at = slice(part * half, (part + 1) * half)
        rows = far[...]
        gate = gate_sum[at, :] + dot(rows, gate_w[...])
        up = up_sum[at, :] + dot(rows, up_w[...])
        active = activate(gate, up)
        across[...] = dot(active, down_far[...]).astype(jnp.bfloat16)
        for k, out in enumerate((for_a, for_b, kept)):
            block = down_near[:, k * quarter : (k + 1) * quarter]
            out[at, :] = dot(active, block).astype(jnp.bfloat16)


def first_call(own, near_a, near_b, gate_w, up_w):
    rows, hidden = own.shape[0], gate_w.shape[1]
    shape = jax.ShapeDtypeStruct((rows, hidden), jnp.float32)
    return pl.pallas_call(
        first_body,
        out_shape=(shape, shape),
        compiler_params=pltpu.CompilerParams(vmem_limit_bytes=VMEM_BYTES),
        cost_estimate=pl.CostEstimate(
            flops=4 * rows * gate_w.shape[0] * hidden, bytes_accessed=8 << 20, transcendentals=0
        ),
        interpret=INTERPRET,
        name="first",
    )(own, near_a, near_b, gate_w, up_w)


def last_call(gate_sum, up_sum, far_a, far_b, gate_w, up_w, down_far, down_near):
    rows, hidden = gate_sum.shape
    half, quarter = far_a.shape
    small = jax.ShapeDtypeStruct((half, quarter), jnp.bfloat16)
    full = jax.ShapeDtypeStruct((rows, quarter), jnp.bfloat16)
    return pl.pallas_call(
        last_body,
        out_shape=(small, small, full, full, full),
        compiler_params=pltpu.CompilerParams(vmem_limit_bytes=VMEM_BYTES),
        cost_estimate=pl.CostEstimate(
            flops=12 * rows * quarter * hidden, bytes_accessed=8 << 20, transcendentals=rows * hidden
        ),
        interpret=INTERPRET,
        name="last",
    )(gate_sum, up_sum, far_a, far_b, gate_w, up_w, down_far, down_near)


def merge_body(for_a, for_b, via_a, via_b, sum_a, sum_b):
    half = via_a.shape[0]
    f32 = jnp.float32
    sum_a[:half, :] = for_a[:half, :]
    sum_a[half:, :] = (for_a[half:, :].astype(f32) + via_b[...].astype(f32)).astype(jnp.bfloat16)
    sum_b[:half, :] = (for_b[:half, :].astype(f32) + via_a[...].astype(f32)).astype(jnp.bfloat16)
    sum_b[half:, :] = for_b[half:, :]


def merge_call(for_a, for_b, via_a, via_b):
    shape = jax.ShapeDtypeStruct(for_a.shape, for_a.dtype)
    return pl.pallas_call(
        merge_body,
        out_shape=(shape, shape),
        compiler_params=pltpu.CompilerParams(vmem_limit_bytes=8 << 20),
        cost_estimate=pl.CostEstimate(flops=1 << 20, bytes_accessed=3 << 20, transcendentals=0),
        interpret=INTERPRET,
        name="merge",
    )(for_a, for_b, via_a, via_b)


def layer(tokens, expert_ids, route_weight, norm_gain, expert_gate, expert_up, expert_down):
    groups = lax.axis_size("ep")
    tp_count = lax.axis_size("tp")
    tok_count, width = tokens.shape
    top_count = expert_ids.shape[1]
    capacity = min(tok_count, 3 * tok_count * top_count // groups)
    quarter = width // tp_count
    bf16 = jnp.bfloat16
    me = lax.axis_index("tp")
    mate_a = me + 1 - 2 * (me % 2)
    mate_b = tp_count - 1 - me
    opposite = (me + 2) % tp_count
    even = [(i, i ^ 1) for i in range(tp_count)]
    odd = [(i, tp_count - 1 - i) for i in range(tp_count)]

    values = tokens.astype(jnp.float32)
    scale = lax.rsqrt(jnp.mean(values * values, axis=-1, keepdims=True) + NORM_EPS)
    own_values = lax.dynamic_slice_in_dim(tokens, me * quarter, quarter, 1).astype(jnp.float32)
    own_gain = lax.dynamic_slice_in_dim(norm_gain, me * quarter, quarter, 0)
    normed = (own_values * scale * own_gain).astype(bf16)

    experts = jnp.arange(groups, dtype=jnp.int32)[:, None]
    ids = expert_ids.T
    weights = route_weight.T
    named = [ids[k][None, :] == experts for k in range(top_count)]
    member = named[0]
    for k in range(1, top_count):
        member = member | named[k]
    earlier = (
        jnp.arange(tok_count, dtype=jnp.int32)[:, None] < jnp.arange(tok_count, dtype=jnp.int32)[None, :]
    ).astype(bf16)
    rank = dot(member.astype(bf16), earlier).astype(jnp.int32)
    rank = jnp.where(member, rank, -1)
    weight = sum(jnp.where(named[k], weights[k][None, :], 0.0) for k in range(top_count))
    weight_high = lax.reduce_precision(weight, 8, 7)
    weight_low = weight - weight_high

    gate_w, up_w, down_w = expert_gate[0], expert_up[0], expert_down[0]

    def rows_of(w, blocks):
        return jnp.concatenate([lax.dynamic_slice_in_dim(w, b * quarter, quarter, 0) for b in blocks], axis=0)

    def cols_of(w, blocks):
        return jnp.concatenate([lax.dynamic_slice_in_dim(w, b * quarter, quarter, 1) for b in blocks], axis=1)

    near_blocks = (me, mate_a, mate_b)
    gate_near, up_near = rows_of(gate_w, near_blocks), rows_of(up_w, near_blocks)
    gate_far, up_far = rows_of(gate_w, (opposite,)), rows_of(up_w, (opposite,))
    down_far, down_near = cols_of(down_w, (opposite,)), cols_of(down_w, (mate_a, mate_b, me))

    chosen_of, sends = [], []
    for first in range(0, capacity, SLOTS):
        slots = first + jnp.arange(SLOTS, dtype=jnp.int32)
        chosen = (rank[:, None, :] == slots[None, :, None]).reshape(groups * SLOTS, tok_count)
        chosen_of.append(chosen)
        sends.append(dot(chosen.astype(bf16), normed).astype(bf16).reshape(groups, SLOTS, quarter))

    combined = jnp.zeros((tok_count, quarter), jnp.float32)
    for chunk, first in enumerate(range(0, capacity, SLOTS)):

        def exchange(x):
            return lax.all_to_all(x, "ep", split_axis=0, concat_axis=0, tiled=True)

        def shift(x, name):
            return lax.ppermute(x, "tp", even if name[1] == "r" else odd)

        chosen, send = chosen_of[chunk], sends[chunk]
        rows = groups * SLOTS
        half = rows // 2
        own = exchange(send).reshape(rows, quarter)
        if chunk == 0:
            own, sends, gate_near, up_near, gate_far, up_far, down_far, down_near = lax.optimization_barrier(
                (own, sends, gate_near, up_near, gate_far, up_far, down_far, down_near)
            )
        near_a = shift(own, "nr")
        near_b = shift(own, "nl")
        far_a = shift(near_b[:half], "fr")
        far_b = shift(near_a[half:], "fl")
        gate_sum, up_sum = first_call(own, near_a, near_b, gate_near, up_near)
        across_a, across_b, for_a, for_b, kept = last_call(
            gate_sum, up_sum, far_a, far_b, gate_far, up_far, down_far, down_near
        )
        f32 = jnp.float32
        via_a = shift(across_a, "ar")
        via_b = shift(across_b, "al")
        for_a, for_b = merge_call(for_a, for_b, via_a, via_b)
        got_a = shift(for_a, "br")
        got_b = shift(for_b, "bl")
        total = kept.astype(f32) + got_a.astype(f32) + got_b.astype(f32)
        result = total.astype(bf16).reshape(groups, SLOTS, quarter)
        returned = exchange(result).reshape(rows, quarter)
        for part in (weight_high, weight_low):
            table = jnp.where(chosen.reshape(groups, SLOTS, tok_count), part[:, None, :], 0.0)
            table = table.reshape(rows, tok_count).astype(bf16)
            combined = combined + lax.dot_general(
                table, returned, (((0,), (0,)), ((), ())), preferred_element_type=jnp.float32
            )
    return combined.astype(bf16)


def solution(mesh):
    return jax.shard_map(
        layer,
        mesh=mesh,
        in_specs=(
            P("ep", None),
            P("ep", None),
            P("ep", None),
            P(),
            P("ep", None, "tp"),
            P("ep", None, "tp"),
            P("ep", "tp", None),
        ),
        out_specs=P("ep", "tp"),
        check_vma=False,
    )
```

```python
import jax
import jax.numpy as jnp
from jax import lax
from jax.experimental import pallas as pl
from jax.experimental.pallas import tpu as pltpu
from jax.sharding import PartitionSpec as P


NORM_EPS = 1e-06
CLAMP_LIMIT = 7.0
SWISH_SCALE = 1.702
SLOTS = 8
VMEM_BYTES = 20 << 20
INTERPRET = False


def activate(gate_sum, up_sum):
    gate_cut = jnp.minimum(gate_sum, CLAMP_LIMIT)
    up_cut = jnp.clip(up_sum, -CLAMP_LIMIT, CLAMP_LIMIT)
    return ((up_cut + 1.0) * gate_cut * jax.nn.sigmoid(SWISH_SCALE * gate_cut)).astype(jnp.bfloat16)


def dot(a, b):
    return jnp.dot(a, b, preferred_element_type=jnp.float32)


def first_body(own, near_a, near_b, gate_w, up_w, gate_out, up_out):
    rows, quarter = own.shape
    step = rows // 2
    for top in range(0, rows, step):
        at = slice(top, top + step)
        for w, out in ((gate_w, gate_out), (up_w, up_out)):
            total = dot(own[at, :], w[:quarter, :])
            total = total + dot(near_a[at, :], w[quarter : 2 * quarter, :])
            out[at, :] = total + dot(near_b[at, :], w[2 * quarter :, :])


def last_body(gate_sum, up_sum, far_a, far_b, gate_w, up_w, down_far, down_near, *outs):
    sent_a, sent_b, rest_a, rest_b, kept = outs
    half, quarter = far_a.shape
    low, high = slice(0, half), slice(half, 2 * half)
    for at, far, places in (
        (low, far_a, ((sent_a, low), (sent_a, high), (rest_b, low), (kept, low))),
        (high, far_b, ((sent_b, low), (rest_a, low), (sent_b, high), (kept, high))),
    ):
        rows = far[...]
        gate = gate_sum[at, :] + dot(rows, gate_w[...])
        up = up_sum[at, :] + dot(rows, up_w[...])
        active = activate(gate, up)
        for k, (out, place) in enumerate(places):
            block = down_far[...] if k == 0 else down_near[:, (k - 1) * quarter : k * quarter]
            out[place, :] = dot(active, block).astype(jnp.bfloat16)


def total_body(kept, got_a, got_b, late_a, late_b, out):
    half = late_a.shape[0]
    f32 = jnp.float32
    top = kept[:half, :].astype(f32) + got_a[half:, :].astype(f32) + late_b[...].astype(f32)
    out[:half, :] = top.astype(jnp.bfloat16)
    bottom = kept[half:, :].astype(f32) + late_a[...].astype(f32) + got_b[half:, :].astype(f32)
    out[half:, :] = bottom.astype(jnp.bfloat16)


def total_call(kept, got_a, got_b, late_a, late_b):
    return pl.pallas_call(
        total_body,
        out_shape=jax.ShapeDtypeStruct(kept.shape, kept.dtype),
        compiler_params=pltpu.CompilerParams(vmem_limit_bytes=8 << 20),
        cost_estimate=pl.CostEstimate(flops=1 << 20, bytes_accessed=3 << 20, transcendentals=0),
        interpret=INTERPRET,
        name="total",
    )(kept, got_a, got_b, late_a, late_b)


def first_call(own, near_a, near_b, gate_w, up_w):
    rows, hidden = own.shape[0], gate_w.shape[1]
    shape = jax.ShapeDtypeStruct((rows, hidden), jnp.float32)
    return pl.pallas_call(
        first_body,
        out_shape=(shape, shape),
        compiler_params=pltpu.CompilerParams(vmem_limit_bytes=VMEM_BYTES),
        cost_estimate=pl.CostEstimate(
            flops=4 * rows * gate_w.shape[0] * hidden, bytes_accessed=8 << 20, transcendentals=0
        ),
        interpret=INTERPRET,
        name="first",
    )(own, near_a, near_b, gate_w, up_w)


def last_call(gate_sum, up_sum, far_a, far_b, gate_w, up_w, down_far, down_near):
    rows, hidden = gate_sum.shape
    half, quarter = far_a.shape
    small = jax.ShapeDtypeStruct((half, quarter), jnp.bfloat16)
    full = jax.ShapeDtypeStruct((rows, quarter), jnp.bfloat16)
    return pl.pallas_call(
        last_body,
        out_shape=(full, full, small, small, full),
        compiler_params=pltpu.CompilerParams(vmem_limit_bytes=VMEM_BYTES),
        cost_estimate=pl.CostEstimate(
            flops=12 * rows * quarter * hidden, bytes_accessed=8 << 20, transcendentals=rows * hidden
        ),
        interpret=INTERPRET,
        name="last",
    )(gate_sum, up_sum, far_a, far_b, gate_w, up_w, down_far, down_near)


def layer(tokens, expert_ids, route_weight, norm_gain, expert_gate, expert_up, expert_down):
    groups = lax.axis_size("ep")
    tp_count = lax.axis_size("tp")
    tok_count, width = tokens.shape
    top_count = expert_ids.shape[1]
    capacity = min(tok_count, 3 * tok_count * top_count // groups)
    quarter = width // tp_count
    bf16 = jnp.bfloat16
    me = lax.axis_index("tp")
    mate_a = me + 1 - 2 * (me % 2)
    mate_b = tp_count - 1 - me
    opposite = (me + 2) % tp_count
    even = [(i, i ^ 1) for i in range(tp_count)]
    odd = [(i, tp_count - 1 - i) for i in range(tp_count)]

    values = tokens.astype(jnp.float32)
    scale = lax.rsqrt(jnp.mean(values * values, axis=-1, keepdims=True) + NORM_EPS)
    own_values = lax.dynamic_slice_in_dim(tokens, me * quarter, quarter, 1).astype(jnp.float32)
    own_gain = lax.dynamic_slice_in_dim(norm_gain, me * quarter, quarter, 0)
    normed = (own_values * scale * own_gain).astype(bf16)

    experts = jnp.arange(groups, dtype=jnp.int32)[:, None]
    ids = expert_ids.T
    weights = route_weight.T
    named = [ids[k][None, :] == experts for k in range(top_count)]
    member = named[0]
    for k in range(1, top_count):
        member = member | named[k]
    earlier = (
        jnp.arange(tok_count, dtype=jnp.int32)[:, None] < jnp.arange(tok_count, dtype=jnp.int32)[None, :]
    ).astype(bf16)
    rank = dot(member.astype(bf16), earlier).astype(jnp.int32)
    rank = jnp.where(member, rank, -1)
    weight = sum(jnp.where(named[k], weights[k][None, :], 0.0) for k in range(top_count))
    weight_high = lax.reduce_precision(weight, 8, 7)
    weight_low = weight - weight_high

    gate_w, up_w, down_w = expert_gate[0], expert_up[0], expert_down[0]

    def rows_of(w, blocks):
        return jnp.concatenate([lax.dynamic_slice_in_dim(w, b * quarter, quarter, 0) for b in blocks], axis=0)

    def cols_of(w, blocks):
        return jnp.concatenate([lax.dynamic_slice_in_dim(w, b * quarter, quarter, 1) for b in blocks], axis=1)

    near_blocks = (me, mate_a, mate_b)
    gate_near, up_near = rows_of(gate_w, near_blocks), rows_of(up_w, near_blocks)
    gate_far, up_far = rows_of(gate_w, (opposite,)), rows_of(up_w, (opposite,))
    down_far, down_near = cols_of(down_w, (opposite,)), cols_of(down_w, (mate_a, mate_b, me))

    tables, sends = [], []
    for first in range(0, capacity, SLOTS):
        slots = first + jnp.arange(SLOTS, dtype=jnp.int32)
        chosen = rank[:, None, :] == slots[None, :, None]
        rows = groups * SLOTS
        tables.append(
            [jnp.where(chosen, p[:, None, :], 0.0).reshape(rows, tok_count).astype(bf16) for p in (weight_high, weight_low)]
        )

    for first, last in ((0, SLOTS), (SLOTS, capacity)):
        slots = jnp.arange(first, last, dtype=jnp.int32)
        chosen = (rank[:, None, :] == slots[None, :, None]).reshape(groups * (last - first), tok_count)
        sends.append(dot(chosen.astype(bf16), normed).astype(bf16))

    combined = jnp.zeros((tok_count, quarter), jnp.float32)
    for chunk, first in enumerate(range(0, capacity, SLOTS)):

        def exchange(x):
            return lax.all_to_all(x, "ep", split_axis=0, concat_axis=0, tiled=True)

        def shift(x, name):
            return lax.ppermute(x, "tp", even if name[1] == "r" else odd)

        half = rows // 2
        if chunk == 0:
            own = exchange(sends[0].reshape(groups, SLOTS, quarter)).reshape(rows, quarter)
            own, sends, tables, gate_near, up_near, gate_far, up_far, down_far, down_near = lax.optimization_barrier(
                (own, sends, tables, gate_near, up_near, gate_far, up_far, down_far, down_near)
            )
        elif chunk == 1:
            rest = exchange(sends[1].reshape(groups, capacity - SLOTS, quarter))
        if chunk:
            own = rest[:, first - SLOTS : first].reshape(rows, quarter)
        near_a = shift(own, "nr")
        near_b = shift(own, "nl")
        far_a = shift(near_b[:half], "fr")
        far_b = shift(near_a[half:], "fl")
        gate_sum, up_sum = first_call(own, near_a, near_b, gate_near, up_near)
        sent_a, sent_b, rest_a, rest_b, kept = last_call(
            gate_sum, up_sum, far_a, far_b, gate_far, up_far, down_far, down_near
        )
        f32 = jnp.float32
        got_a = shift(sent_a, "ar")
        got_b = shift(sent_b, "al")
        late_a = shift((rest_a.astype(f32) + got_b[:half].astype(f32)).astype(bf16), "br")
        late_b = shift((rest_b.astype(f32) + got_a[:half].astype(f32)).astype(bf16), "bl")
        result = total_call(kept, got_a, got_b, late_a, late_b).reshape(groups, SLOTS, quarter)
        returned = exchange(result).reshape(rows, quarter)
        table_high, table_low = tables[chunk]
        added = lax.dot_general(table_high, returned, (((0,), (0,)), ((), ())), preferred_element_type=jnp.float32)
        combined = combined + added
        added = lax.dot_general(table_low, returned, (((0,), (0,)), ((), ())), preferred_element_type=jnp.float32)
        combined = combined + added
        if first + SLOTS < capacity:
            combined = lax.optimization_barrier(combined)
    return combined.astype(bf16)


def solution(mesh):
    return jax.shard_map(
        layer,
        mesh=mesh,
        in_specs=(
            P("ep", None),
            P("ep", None),
            P("ep", None),
            P(),
            P("ep", None, "tp"),
            P("ep", None, "tp"),
            P("ep", "tp", None),
        ),
        out_specs=P("ep", "tp"),
        check_vma=False,
    )
```

```python
import jax
import jax.numpy as jnp
from jax import lax
from jax.experimental import pallas as pl
from jax.experimental.pallas import tpu as pltpu
from jax.sharding import PartitionSpec as P


NORM_EPS = 1e-06
CLAMP_LIMIT = 7.0
SWISH_SCALE = 1.702
SLOTS = 8
VMEM_BYTES = 20 << 20
INTERPRET = False


def activate(gate_sum, up_sum):
    gate_cut = jnp.minimum(gate_sum, CLAMP_LIMIT)
    up_cut = jnp.clip(up_sum, -CLAMP_LIMIT, CLAMP_LIMIT)
    return ((up_cut + 1.0) * gate_cut * jax.nn.sigmoid(SWISH_SCALE * gate_cut)).astype(jnp.bfloat16)


def dot(a, b):
    return jnp.dot(a, b, preferred_element_type=jnp.float32)


def prepare_body(me, tokens, gain, ids, normed_out, rank_out, send_out):
    tok_count, width = tokens.shape
    quarter = normed_out.shape[1]
    groups = rank_out.shape[0]
    rows = send_out.shape[0]
    f32, bf16 = jnp.float32, jnp.bfloat16
    values = tokens[...].astype(f32)
    scale = lax.rsqrt(jnp.sum(values * values, axis=1, keepdims=True) / width + NORM_EPS)
    at = pl.ds(pl.multiple_of(me[0] * quarter, quarter), quarter)
    normed = (tokens[:, at].astype(f32) * scale * gain[:, at]).astype(bf16)
    normed_out[...] = normed
    experts = lax.broadcasted_iota(jnp.int32, (groups, tok_count), 0)
    member = experts == ids[0:1, :]
    for k in range(1, ids.shape[0]):
        member = member | (experts == ids[k : k + 1, :])
    shape = (tok_count, tok_count)
    earlier = lax.broadcasted_iota(jnp.int32, shape, 0) < lax.broadcasted_iota(jnp.int32, shape, 1)
    rank = dot(member.astype(f32).astype(bf16), earlier.astype(f32).astype(bf16))
    rank = jnp.where(member, rank, -1.0)
    rank_out[...] = rank.astype(jnp.int32)
    spread = lax.broadcasted_iota(jnp.int32, (rows, groups), 0) // SLOTS
    spread = (spread == lax.broadcasted_iota(jnp.int32, (rows, groups), 1)).astype(f32).astype(bf16)
    slot = (lax.broadcasted_iota(jnp.int32, (rows, tok_count), 0) % SLOTS).astype(f32)
    chosen = (dot(spread, rank.astype(bf16)) == slot).astype(f32).astype(bf16)
    send_out[...] = dot(chosen, normed).astype(bf16)


def prepare_call(me, tokens, gain, ids, quarter, groups):
    tok_count = tokens.shape[0]
    vmem = pl.BlockSpec(memory_space=pltpu.VMEM)
    return pl.pallas_call(
        prepare_body,
        out_shape=(
            jax.ShapeDtypeStruct((tok_count, quarter), jnp.bfloat16),
            jax.ShapeDtypeStruct((groups, tok_count), jnp.int32),
            jax.ShapeDtypeStruct((groups * SLOTS, quarter), jnp.bfloat16),
        ),
        in_specs=[pl.BlockSpec(memory_space=pltpu.SMEM), vmem, vmem, vmem],
        compiler_params=pltpu.CompilerParams(vmem_limit_bytes=VMEM_BYTES),
        interpret=INTERPRET,
        name="prepare",
    )(me.reshape(1), tokens, gain.reshape(1, -1), ids)


def first_body(own, near_a, near_b, gate_w, up_w, gate_out, up_out):
    rows, quarter = own.shape
    step = rows // 2
    for top in range(0, rows, step):
        at = slice(top, top + step)
        for w, out in ((gate_w, gate_out), (up_w, up_out)):
            total = dot(own[at, :], w[:quarter, :])
            total = total + dot(near_a[at, :], w[quarter : 2 * quarter, :])
            out[at, :] = total + dot(near_b[at, :], w[2 * quarter :, :])


def last_body(gate_sum, up_sum, far_a, far_b, gate_w, up_w, down_far, down_near, *outs):
    sent_a, sent_b, rest_a, rest_b, kept = outs
    half, quarter = far_a.shape
    low, high = slice(0, half), slice(half, 2 * half)
    for at, far, places in (
        (low, far_a, ((sent_a, low), (sent_a, high), (rest_b, low), (kept, low))),
        (high, far_b, ((sent_b, low), (rest_a, low), (sent_b, high), (kept, high))),
    ):
        rows = far[...]
        gate = gate_sum[at, :] + dot(rows, gate_w[...])
        up = up_sum[at, :] + dot(rows, up_w[...])
        active = activate(gate, up)
        for k, (out, place) in enumerate(places):
            block = down_far[...] if k == 0 else down_near[:, (k - 1) * quarter : k * quarter]
            out[place, :] = dot(active, block).astype(jnp.bfloat16)


def total_body(kept, got_a, got_b, late_a, late_b, out):
    half = late_a.shape[0]
    f32 = jnp.float32
    top = kept[:half, :].astype(f32) + got_a[half:, :].astype(f32) + late_b[...].astype(f32)
    out[:half, :] = top.astype(jnp.bfloat16)
    bottom = kept[half:, :].astype(f32) + late_a[...].astype(f32) + got_b[half:, :].astype(f32)
    out[half:, :] = bottom.astype(jnp.bfloat16)


def total_call(kept, got_a, got_b, late_a, late_b):
    return pl.pallas_call(
        total_body,
        out_shape=jax.ShapeDtypeStruct(kept.shape, kept.dtype),
        compiler_params=pltpu.CompilerParams(vmem_limit_bytes=8 << 20),
        cost_estimate=pl.CostEstimate(flops=1 << 20, bytes_accessed=3 << 20, transcendentals=0),
        interpret=INTERPRET,
        name="total",
    )(kept, got_a, got_b, late_a, late_b)


def first_call(own, near_a, near_b, gate_w, up_w):
    rows, hidden = own.shape[0], gate_w.shape[1]
    shape = jax.ShapeDtypeStruct((rows, hidden), jnp.float32)
    return pl.pallas_call(
        first_body,
        out_shape=(shape, shape),
        compiler_params=pltpu.CompilerParams(vmem_limit_bytes=VMEM_BYTES),
        cost_estimate=pl.CostEstimate(
            flops=4 * rows * gate_w.shape[0] * hidden, bytes_accessed=8 << 20, transcendentals=0
        ),
        interpret=INTERPRET,
        name="first",
    )(own, near_a, near_b, gate_w, up_w)


def last_call(gate_sum, up_sum, far_a, far_b, gate_w, up_w, down_far, down_near):
    rows, hidden = gate_sum.shape
    half, quarter = far_a.shape
    small = jax.ShapeDtypeStruct((half, quarter), jnp.bfloat16)
    full = jax.ShapeDtypeStruct((rows, quarter), jnp.bfloat16)
    return pl.pallas_call(
        last_body,
        out_shape=(full, full, small, small, full),
        compiler_params=pltpu.CompilerParams(vmem_limit_bytes=VMEM_BYTES),
        cost_estimate=pl.CostEstimate(
            flops=12 * rows * quarter * hidden, bytes_accessed=8 << 20, transcendentals=rows * hidden
        ),
        interpret=INTERPRET,
        name="last",
    )(gate_sum, up_sum, far_a, far_b, gate_w, up_w, down_far, down_near)


def layer(tokens, expert_ids, route_weight, norm_gain, expert_gate, expert_up, expert_down):
    groups = lax.axis_size("ep")
    tp_count = lax.axis_size("tp")
    tok_count, width = tokens.shape
    top_count = expert_ids.shape[1]
    capacity = min(tok_count, 3 * tok_count * top_count // groups)
    quarter = width // tp_count
    bf16 = jnp.bfloat16
    me = lax.axis_index("tp")
    mate_a = me + 1 - 2 * (me % 2)
    mate_b = tp_count - 1 - me
    opposite = (me + 2) % tp_count
    even = [(i, i ^ 1) for i in range(tp_count)]
    odd = [(i, tp_count - 1 - i) for i in range(tp_count)]

    normed, rank, first_send = prepare_call(me, tokens, norm_gain, expert_ids.T, quarter, groups)
    experts = jnp.arange(groups, dtype=jnp.int32)[:, None]
    ids = expert_ids.T
    weights = route_weight.T
    named = [ids[k][None, :] == experts for k in range(top_count)]
    weight = sum(jnp.where(named[k], weights[k][None, :], 0.0) for k in range(top_count))
    weight_high = lax.reduce_precision(weight, 8, 7)
    weight_low = weight - weight_high

    gate_w, up_w, down_w = expert_gate[0], expert_up[0], expert_down[0]

    def rows_of(w, blocks):
        return jnp.concatenate([lax.dynamic_slice_in_dim(w, b * quarter, quarter, 0) for b in blocks], axis=0)

    def cols_of(w, blocks):
        return jnp.concatenate([lax.dynamic_slice_in_dim(w, b * quarter, quarter, 1) for b in blocks], axis=1)

    near_blocks = (me, mate_a, mate_b)
    gate_near, up_near = rows_of(gate_w, near_blocks), rows_of(up_w, near_blocks)
    gate_far, up_far = rows_of(gate_w, (opposite,)), rows_of(up_w, (opposite,))
    down_far, down_near = cols_of(down_w, (opposite,)), cols_of(down_w, (mate_a, mate_b, me))

    tables = []
    for first in range(0, capacity, SLOTS):
        slots = first + jnp.arange(SLOTS, dtype=jnp.int32)
        chosen = rank[:, None, :] == slots[None, :, None]
        rows = groups * SLOTS
        tables.append(
            [jnp.where(chosen, p[:, None, :], 0.0).reshape(rows, tok_count).astype(bf16) for p in (weight_high, weight_low)]
        )

    slots = jnp.arange(SLOTS, capacity, dtype=jnp.int32)
    chosen = (rank[:, None, :] == slots[None, :, None]).reshape(groups * (capacity - SLOTS), tok_count)
    sends = [first_send, dot(chosen.astype(bf16), normed).astype(bf16)]

    combined = jnp.zeros((tok_count, quarter), jnp.float32)
    for chunk, first in enumerate(range(0, capacity, SLOTS)):

        def exchange(x):
            return lax.all_to_all(x, "ep", split_axis=0, concat_axis=0, tiled=True)

        def shift(x, name):
            return lax.ppermute(x, "tp", even if name[1] == "r" else odd)

        half = rows // 2
        if chunk == 0:
            own = exchange(sends[0].reshape(groups, SLOTS, quarter)).reshape(rows, quarter)
            own, sends, tables, gate_near, up_near, gate_far, up_far, down_far, down_near = lax.optimization_barrier(
                (own, sends, tables, gate_near, up_near, gate_far, up_far, down_far, down_near)
            )
        elif chunk == 1:
            rest = exchange(sends[1].reshape(groups, capacity - SLOTS, quarter))
        if chunk:
            own = rest[:, first - SLOTS : first].reshape(rows, quarter)
        near_a = shift(own, "nr")
        near_b = shift(own, "nl")
        far_a = shift(near_b[:half], "fr")
        far_b = shift(near_a[half:], "fl")
        gate_sum, up_sum = first_call(own, near_a, near_b, gate_near, up_near)
        sent_a, sent_b, rest_a, rest_b, kept = last_call(
            gate_sum, up_sum, far_a, far_b, gate_far, up_far, down_far, down_near
        )
        f32 = jnp.float32
        got_a = shift(sent_a, "ar")
        got_b = shift(sent_b, "al")
        late_a = shift((rest_a.astype(f32) + got_b[:half].astype(f32)).astype(bf16), "br")
        late_b = shift((rest_b.astype(f32) + got_a[:half].astype(f32)).astype(bf16), "bl")
        result = total_call(kept, got_a, got_b, late_a, late_b).reshape(groups, SLOTS, quarter)
        returned = exchange(result).reshape(rows, quarter)
        table_high, table_low = tables[chunk]
        added = lax.dot_general(table_high, returned, (((0,), (0,)), ((), ())), preferred_element_type=jnp.float32)
        combined = combined + added
        added = lax.dot_general(table_low, returned, (((0,), (0,)), ((), ())), preferred_element_type=jnp.float32)
        combined = combined + added
        if first + SLOTS < capacity:
            combined = lax.optimization_barrier(combined)
    return combined.astype(bf16)


def solution(mesh):
    return jax.shard_map(
        layer,
        mesh=mesh,
        in_specs=(
            P("ep", None),
            P("ep", None),
            P("ep", None),
            P(),
            P("ep", None, "tp"),
            P("ep", None, "tp"),
            P("ep", "tp", None),
        ),
        out_specs=P("ep", "tp"),
        check_vma=False,
    )
```

```python
import jax
import jax.numpy as jnp
from jax import lax
from jax.experimental import pallas as pl
from jax.experimental.pallas import tpu as pltpu
from jax.sharding import PartitionSpec as P


NORM_EPS = 1e-06
CLAMP_LIMIT = 7.0
SWISH_SCALE = 1.702
SLOTS = 8
VMEM_BYTES = 20 << 20
INTERPRET = False


def activate(gate_sum, up_sum):
    gate_cut = jnp.minimum(gate_sum, CLAMP_LIMIT)
    up_cut = jnp.clip(up_sum, -CLAMP_LIMIT, CLAMP_LIMIT)
    return ((up_cut + 1.0) * gate_cut * jax.nn.sigmoid(SWISH_SCALE * gate_cut)).astype(jnp.bfloat16)


def dot(a, b):
    return jnp.dot(a, b, preferred_element_type=jnp.float32)


def prepare_body(me, tokens, gain, ids, normed_out, rank_out, send_out):
    tok_count, width = tokens.shape
    quarter = normed_out.shape[1]
    groups = rank_out.shape[0]
    rows = send_out.shape[0]
    f32, bf16 = jnp.float32, jnp.bfloat16
    values = tokens[...].astype(f32)
    scale = lax.rsqrt(jnp.sum(values * values, axis=1, keepdims=True) / width + NORM_EPS)
    at = pl.ds(pl.multiple_of(me[0] * quarter, quarter), quarter)
    normed = (tokens[:, at].astype(f32) * scale * gain[:, at]).astype(bf16)
    normed_out[...] = normed
    experts = lax.broadcasted_iota(jnp.int32, (groups, tok_count), 0)
    member = experts == ids[0:1, :]
    for k in range(1, ids.shape[0]):
        member = member | (experts == ids[k : k + 1, :])
    shape = (tok_count, tok_count)
    earlier = lax.broadcasted_iota(jnp.int32, shape, 0) < lax.broadcasted_iota(jnp.int32, shape, 1)
    rank = dot(member.astype(f32).astype(bf16), earlier.astype(f32).astype(bf16))
    rank = jnp.where(member, rank, -1.0)
    rank_out[...] = rank.astype(jnp.int32)
    spread = lax.broadcasted_iota(jnp.int32, (rows, groups), 0) // SLOTS
    spread = (spread == lax.broadcasted_iota(jnp.int32, (rows, groups), 1)).astype(f32).astype(bf16)
    slot = (lax.broadcasted_iota(jnp.int32, (rows, tok_count), 0) % SLOTS).astype(f32)
    chosen = (dot(spread, rank.astype(bf16)) == slot).astype(f32).astype(bf16)
    send_out[...] = dot(chosen, normed).astype(bf16)


def prepare_call(me, tokens, gain, ids, quarter, groups):
    tok_count = tokens.shape[0]
    if not INTERPRET:
        tokens, gain, ids = (pltpu.with_memory_space_constraint(x, pltpu.HBM) for x in (tokens, gain.reshape(1, -1), ids))
    return pl.pallas_call(
        prepare_body,
        out_shape=(
            jax.ShapeDtypeStruct((tok_count, quarter), jnp.bfloat16),
            jax.ShapeDtypeStruct((groups, tok_count), jnp.int32),
            jax.ShapeDtypeStruct((groups * SLOTS, quarter), jnp.bfloat16),
        ),
        in_specs=[pl.BlockSpec(memory_space=pltpu.SMEM), pl.BlockSpec(), pl.BlockSpec(), pl.BlockSpec()],
        compiler_params=pltpu.CompilerParams(vmem_limit_bytes=VMEM_BYTES),
        interpret=INTERPRET,
        name="prepare",
    )(me.reshape(1), tokens, gain.reshape(1, -1), ids)


def first_body(own, near_a, near_b, gate_w, up_w, gate_out, up_out):
    rows, quarter = own.shape
    step = rows // 2
    for top in range(0, rows, step):
        at = slice(top, top + step)
        for w, out in ((gate_w, gate_out), (up_w, up_out)):
            total = dot(own[at, :], w[:quarter, :])
            total = total + dot(near_a[at, :], w[quarter : 2 * quarter, :])
            out[at, :] = total + dot(near_b[at, :], w[2 * quarter :, :])


def last_body(gate_sum, up_sum, far_a, far_b, gate_w, up_w, down_far, down_near, *outs):
    sent_a, sent_b, rest_a, rest_b, kept = outs
    half, quarter = far_a.shape
    low, high = slice(0, half), slice(half, 2 * half)
    for at, far, places in (
        (low, far_a, ((sent_a, low), (sent_a, high), (rest_b, low), (kept, low))),
        (high, far_b, ((sent_b, low), (rest_a, low), (sent_b, high), (kept, high))),
    ):
        rows = far[...]
        gate = gate_sum[at, :] + dot(rows, gate_w[...])
        up = up_sum[at, :] + dot(rows, up_w[...])
        active = activate(gate, up)
        for k, (out, place) in enumerate(places):
            block = down_far[...] if k == 0 else down_near[:, (k - 1) * quarter : k * quarter]
            out[place, :] = dot(active, block).astype(jnp.bfloat16)


def total_body(kept, got_a, got_b, late_a, late_b, out):
    half = late_a.shape[0]
    f32 = jnp.float32
    top = kept[:half, :].astype(f32) + got_a[half:, :].astype(f32) + late_b[...].astype(f32)
    out[:half, :] = top.astype(jnp.bfloat16)
    bottom = kept[half:, :].astype(f32) + late_a[...].astype(f32) + got_b[half:, :].astype(f32)
    out[half:, :] = bottom.astype(jnp.bfloat16)


def total_call(kept, got_a, got_b, late_a, late_b):
    return pl.pallas_call(
        total_body,
        out_shape=jax.ShapeDtypeStruct(kept.shape, kept.dtype),
        compiler_params=pltpu.CompilerParams(vmem_limit_bytes=8 << 20),
        cost_estimate=pl.CostEstimate(flops=1 << 20, bytes_accessed=3 << 20, transcendentals=0),
        interpret=INTERPRET,
        name="total",
    )(kept, got_a, got_b, late_a, late_b)


def first_call(own, near_a, near_b, gate_w, up_w):
    rows, hidden = own.shape[0], gate_w.shape[1]
    shape = jax.ShapeDtypeStruct((rows, hidden), jnp.float32)
    return pl.pallas_call(
        first_body,
        out_shape=(shape, shape),
        compiler_params=pltpu.CompilerParams(vmem_limit_bytes=VMEM_BYTES),
        cost_estimate=pl.CostEstimate(
            flops=4 * rows * gate_w.shape[0] * hidden, bytes_accessed=8 << 20, transcendentals=0
        ),
        interpret=INTERPRET,
        name="first",
    )(own, near_a, near_b, gate_w, up_w)


def last_call(gate_sum, up_sum, far_a, far_b, gate_w, up_w, down_far, down_near):
    rows, hidden = gate_sum.shape
    half, quarter = far_a.shape
    shape_of = jax.ShapeDtypeStruct if INTERPRET else pltpu.HBM
    small = shape_of((half, quarter), jnp.bfloat16)
    kept = shape_of((rows, quarter), jnp.bfloat16)
    full = jax.ShapeDtypeStruct((rows, quarter), jnp.bfloat16)
    return pl.pallas_call(
        last_body,
        out_shape=(full, full, small, small, kept),
        compiler_params=pltpu.CompilerParams(vmem_limit_bytes=VMEM_BYTES),
        cost_estimate=pl.CostEstimate(
            flops=12 * rows * quarter * hidden, bytes_accessed=8 << 20, transcendentals=rows * hidden
        ),
        interpret=INTERPRET,
        name="last",
    )(gate_sum, up_sum, far_a, far_b, gate_w, up_w, down_far, down_near)


def layer(tokens, expert_ids, route_weight, norm_gain, expert_gate, expert_up, expert_down):
    groups = lax.axis_size("ep")
    tp_count = lax.axis_size("tp")
    tok_count, width = tokens.shape
    top_count = expert_ids.shape[1]
    capacity = min(tok_count, 3 * tok_count * top_count // groups)
    quarter = width // tp_count
    bf16 = jnp.bfloat16
    me = lax.axis_index("tp")
    mate_a = me + 1 - 2 * (me % 2)
    mate_b = tp_count - 1 - me
    opposite = (me + 2) % tp_count
    even = [(i, i ^ 1) for i in range(tp_count)]
    odd = [(i, tp_count - 1 - i) for i in range(tp_count)]

    normed, rank, first_send = prepare_call(me, tokens, norm_gain, expert_ids.T, quarter, groups)
    experts = jnp.arange(groups, dtype=jnp.int32)[:, None]
    ids = expert_ids.T
    weights = route_weight.T
    named = [ids[k][None, :] == experts for k in range(top_count)]
    weight = sum(jnp.where(named[k], weights[k][None, :], 0.0) for k in range(top_count))
    weight_high = lax.reduce_precision(weight, 8, 7)
    weight_low = weight - weight_high

    gate_w, up_w, down_w = expert_gate[0], expert_up[0], expert_down[0]

    def rows_of(w, blocks):
        return jnp.concatenate([lax.dynamic_slice_in_dim(w, b * quarter, quarter, 0) for b in blocks], axis=0)

    def cols_of(w, blocks):
        return jnp.concatenate([lax.dynamic_slice_in_dim(w, b * quarter, quarter, 1) for b in blocks], axis=1)

    near_blocks = (me, mate_a, mate_b)
    gate_near, up_near = rows_of(gate_w, near_blocks), rows_of(up_w, near_blocks)
    gate_far, up_far = rows_of(gate_w, (opposite,)), rows_of(up_w, (opposite,))
    down_far, down_near = cols_of(down_w, (opposite,)), cols_of(down_w, (mate_a, mate_b, me))

    tables = []
    for first in range(0, capacity, SLOTS):
        slots = first + jnp.arange(SLOTS, dtype=jnp.int32)
        chosen = rank[:, None, :] == slots[None, :, None]
        rows = groups * SLOTS
        tables.append(
            [jnp.where(chosen, p[:, None, :], 0.0).reshape(rows, tok_count).astype(bf16) for p in (weight_high, weight_low)]
        )

    slots = jnp.arange(SLOTS, capacity, dtype=jnp.int32)
    chosen = (rank[:, None, :] == slots[None, :, None]).reshape(groups * (capacity - SLOTS), tok_count)
    sends = [first_send, dot(chosen.astype(bf16), normed).astype(bf16)]

    combined = jnp.zeros((tok_count, quarter), jnp.float32)
    for chunk, first in enumerate(range(0, capacity, SLOTS)):

        def exchange(x):
            return lax.all_to_all(x, "ep", split_axis=0, concat_axis=0, tiled=True)

        def shift(x, name):
            return lax.ppermute(x, "tp", even if name[1] == "r" else odd)

        half = rows // 2
        if chunk == 0:
            own = exchange(sends[0].reshape(groups, SLOTS, quarter)).reshape(rows, quarter)
            own, sends, tables, gate_near, up_near, gate_far, up_far, down_far, down_near = lax.optimization_barrier(
                (own, sends, tables, gate_near, up_near, gate_far, up_far, down_far, down_near)
            )
        elif chunk == 1:
            rest = exchange(sends[1].reshape(groups, capacity - SLOTS, quarter))
        if chunk:
            own = rest[:, first - SLOTS : first].reshape(rows, quarter)
        near_a = shift(own, "nr")
        near_b = shift(own, "nl")
        far_a = shift(near_b[:half], "fr")
        far_b = shift(near_a[half:], "fl")
        gate_sum, up_sum = first_call(own, near_a, near_b, gate_near, up_near)
        sent_a, sent_b, rest_a, rest_b, kept = last_call(
            gate_sum, up_sum, far_a, far_b, gate_far, up_far, down_far, down_near
        )
        f32 = jnp.float32
        got_a = shift(sent_a, "ar")
        got_b = shift(sent_b, "al")
        late_a = shift((rest_a.astype(f32) + got_b[:half].astype(f32)).astype(bf16), "br")
        late_b = shift((rest_b.astype(f32) + got_a[:half].astype(f32)).astype(bf16), "bl")
        result = total_call(kept, got_a, got_b, late_a, late_b).reshape(groups, SLOTS, quarter)
        returned = exchange(result).reshape(rows, quarter)
        table_high, table_low = tables[chunk]
        added = lax.dot_general(table_high, returned, (((0,), (0,)), ((), ())), preferred_element_type=jnp.float32)
        combined = combined + added
        added = lax.dot_general(table_low, returned, (((0,), (0,)), ((), ())), preferred_element_type=jnp.float32)
        combined = combined + added
        if first + SLOTS < capacity:
            combined = lax.optimization_barrier(combined)
    return combined.astype(bf16)


def solution(mesh):
    return jax.shard_map(
        layer,
        mesh=mesh,
        in_specs=(
            P("ep", None),
            P("ep", None),
            P("ep", None),
            P(),
            P("ep", None, "tp"),
            P("ep", None, "tp"),
            P("ep", "tp", None),
        ),
        out_specs=P("ep", "tp"),
        check_vma=False,
    )
```

```python
import jax
import jax.numpy as jnp
from jax import lax
from jax.experimental import pallas as pl
from jax.experimental.pallas import tpu as pltpu
from jax.sharding import PartitionSpec as P


NORM_EPS = 1e-06
CLAMP_LIMIT = 7.0
SWISH_SCALE = 1.702
SLOTS = 8
VMEM_BYTES = 20 << 20
INTERPRET = False


def activate(gate_sum, up_sum):
    gate_cut = jnp.minimum(gate_sum, CLAMP_LIMIT)
    up_cut = jnp.clip(up_sum, -CLAMP_LIMIT, CLAMP_LIMIT)
    return ((up_cut + 1.0) * gate_cut * jax.nn.sigmoid(SWISH_SCALE * gate_cut)).astype(jnp.bfloat16)


def dot(a, b):
    return jnp.dot(a, b, preferred_element_type=jnp.float32)


def prepare_body(me, tokens, gain, ids, normed_out, rank_out, send_out):
    tok_count, width = tokens.shape
    quarter = normed_out.shape[1]
    groups = rank_out.shape[0]
    rows = send_out.shape[0]
    f32, bf16 = jnp.float32, jnp.bfloat16
    values = tokens[...].astype(f32)
    scale = lax.rsqrt(jnp.sum(values * values, axis=1, keepdims=True) / width + NORM_EPS)
    at = pl.ds(pl.multiple_of(me[0] * quarter, quarter), quarter)
    normed = (tokens[:, at].astype(f32) * scale * gain[:, at]).astype(bf16)
    normed_out[...] = normed
    experts = lax.broadcasted_iota(jnp.int32, (groups, tok_count), 0)
    member = experts == ids[0:1, :]
    for k in range(1, ids.shape[0]):
        member = member | (experts == ids[k : k + 1, :])
    shape = (tok_count, tok_count)
    earlier = lax.broadcasted_iota(jnp.int32, shape, 0) < lax.broadcasted_iota(jnp.int32, shape, 1)
    rank = dot(member.astype(f32).astype(bf16), earlier.astype(f32).astype(bf16))
    rank = jnp.where(member, rank, -1.0)
    rank_out[...] = rank.astype(jnp.int32)
    spread = lax.broadcasted_iota(jnp.int32, (rows, groups), 0) // SLOTS
    spread = (spread == lax.broadcasted_iota(jnp.int32, (rows, groups), 1)).astype(f32).astype(bf16)
    slot = (lax.broadcasted_iota(jnp.int32, (rows, tok_count), 0) % SLOTS).astype(f32)
    chosen = (dot(spread, rank.astype(bf16)) == slot).astype(f32).astype(bf16)
    send_out[...] = dot(chosen, normed).astype(bf16)


def prepare_call(me, tokens, gain, ids, quarter, groups):
    tok_count = tokens.shape[0]
    if not INTERPRET:
        tokens, gain, ids = (pltpu.with_memory_space_constraint(x, pltpu.HBM) for x in (tokens, gain.reshape(1, -1), ids))
    return pl.pallas_call(
        prepare_body,
        out_shape=(
            jax.ShapeDtypeStruct((tok_count, quarter), jnp.bfloat16),
            jax.ShapeDtypeStruct((groups, tok_count), jnp.int32),
            jax.ShapeDtypeStruct((groups * SLOTS, quarter), jnp.bfloat16),
        ),
        in_specs=[pl.BlockSpec(memory_space=pltpu.SMEM), pl.BlockSpec(), pl.BlockSpec(), pl.BlockSpec()],
        compiler_params=pltpu.CompilerParams(vmem_limit_bytes=VMEM_BYTES),
        interpret=INTERPRET,
        name="prepare",
    )(me.reshape(1), tokens, gain.reshape(1, -1), ids)


def first_body(own, near_a, near_b, gate_w, up_w, gate_out, up_out):
    rows, quarter = own.shape
    step = rows // 2
    for top in range(0, rows, step):
        at = slice(top, top + step)
        for w, out in ((gate_w, gate_out), (up_w, up_out)):
            total = dot(own[at, :], w[:quarter, :])
            total = total + dot(near_a[at, :], w[quarter : 2 * quarter, :])
            out[at, :] = total + dot(near_b[at, :], w[2 * quarter :, :])


def last_body(gate_sum, up_sum, far_a, far_b, gate_w, up_w, down_far, down_near, *outs):
    sent_a, sent_b, rest_a, rest_b, kept = outs
    half, quarter = far_a.shape
    low, high = slice(0, half), slice(half, 2 * half)
    for at, far, places in (
        (low, far_a, ((sent_a, low), (sent_a, high), (rest_b, low), (kept, low))),
        (high, far_b, ((sent_b, low), (rest_a, low), (sent_b, high), (kept, high))),
    ):
        rows = far[...]
        gate = gate_sum[at, :] + dot(rows, gate_w[...])
        up = up_sum[at, :] + dot(rows, up_w[...])
        active = activate(gate, up)
        for k, (out, place) in enumerate(places):
            block = down_far[...] if k == 0 else down_near[:, (k - 1) * quarter : k * quarter]
            out[place, :] = dot(active, block).astype(jnp.bfloat16)


def total_body(kept, got_a, got_b, late_a, late_b, out):
    half = late_a.shape[0]
    f32 = jnp.float32
    top = kept[:half, :].astype(f32) + got_a[...].astype(f32) + late_b[...].astype(f32)
    out[:half, :] = top.astype(jnp.bfloat16)
    bottom = kept[half:, :].astype(f32) + late_a[...].astype(f32) + got_b[...].astype(f32)
    out[half:, :] = bottom.astype(jnp.bfloat16)


def total_call(kept, got_a, got_b, late_a, late_b):
    whole = pl.BlockSpec(kept.shape, lambda i: (0, 0))
    first = pl.BlockSpec(late_a.shape, lambda i: (0, 0))
    second = pl.BlockSpec(late_a.shape, lambda i: (1, 0))
    return pl.pallas_call(
        total_body,
        grid=(1,),
        in_specs=[whole, second, second, first, first],
        out_specs=whole,
        out_shape=jax.ShapeDtypeStruct(kept.shape, kept.dtype),
        compiler_params=pltpu.CompilerParams(vmem_limit_bytes=8 << 20),
        cost_estimate=pl.CostEstimate(flops=1 << 20, bytes_accessed=3 << 20, transcendentals=0),
        interpret=INTERPRET,
        name="total",
    )(kept, got_a, got_b, late_a, late_b)


def first_call(own, near_a, near_b, gate_w, up_w):
    rows, hidden = own.shape[0], gate_w.shape[1]
    shape = jax.ShapeDtypeStruct((rows, hidden), jnp.float32)
    return pl.pallas_call(
        first_body,
        out_shape=(shape, shape),
        compiler_params=pltpu.CompilerParams(vmem_limit_bytes=VMEM_BYTES),
        cost_estimate=pl.CostEstimate(
            flops=4 * rows * gate_w.shape[0] * hidden, bytes_accessed=8 << 20, transcendentals=0
        ),
        interpret=INTERPRET,
        name="first",
    )(own, near_a, near_b, gate_w, up_w)


def last_call(gate_sum, up_sum, far_a, far_b, gate_w, up_w, down_far, down_near):
    rows, hidden = gate_sum.shape
    half, quarter = far_a.shape
    shape_of = jax.ShapeDtypeStruct if INTERPRET else pltpu.HBM
    small = shape_of((half, quarter), jnp.bfloat16)
    kept = shape_of((rows, quarter), jnp.bfloat16)
    full = jax.ShapeDtypeStruct((rows, quarter), jnp.bfloat16)
    return pl.pallas_call(
        last_body,
        out_shape=(full, full, small, small, kept),
        compiler_params=pltpu.CompilerParams(vmem_limit_bytes=VMEM_BYTES),
        cost_estimate=pl.CostEstimate(
            flops=12 * rows * quarter * hidden, bytes_accessed=8 << 20, transcendentals=rows * hidden
        ),
        interpret=INTERPRET,
        name="last",
    )(gate_sum, up_sum, far_a, far_b, gate_w, up_w, down_far, down_near)


def layer(tokens, expert_ids, route_weight, norm_gain, expert_gate, expert_up, expert_down):
    groups = lax.axis_size("ep")
    tp_count = lax.axis_size("tp")
    tok_count, width = tokens.shape
    top_count = expert_ids.shape[1]
    capacity = min(tok_count, 3 * tok_count * top_count // groups)
    quarter = width // tp_count
    bf16 = jnp.bfloat16
    me = lax.axis_index("tp")
    mate_a = me + 1 - 2 * (me % 2)
    mate_b = tp_count - 1 - me
    opposite = (me + 2) % tp_count
    even = [(i, i ^ 1) for i in range(tp_count)]
    odd = [(i, tp_count - 1 - i) for i in range(tp_count)]

    normed, rank, first_send = prepare_call(me, tokens, norm_gain, expert_ids.T, quarter, groups)
    experts = jnp.arange(groups, dtype=jnp.int32)[:, None]
    ids = expert_ids.T
    weights = route_weight.T
    named = [ids[k][None, :] == experts for k in range(top_count)]
    weight = sum(jnp.where(named[k], weights[k][None, :], 0.0) for k in range(top_count))
    weight_high = lax.reduce_precision(weight, 8, 7)
    weight_low = weight - weight_high

    gate_w, up_w, down_w = expert_gate[0], expert_up[0], expert_down[0]

    def rows_of(w, blocks):
        return jnp.concatenate([lax.dynamic_slice_in_dim(w, b * quarter, quarter, 0) for b in blocks], axis=0)

    def cols_of(w, blocks):
        return jnp.concatenate([lax.dynamic_slice_in_dim(w, b * quarter, quarter, 1) for b in blocks], axis=1)

    near_blocks = (me, mate_a, mate_b)
    gate_near, up_near = rows_of(gate_w, near_blocks), rows_of(up_w, near_blocks)
    gate_far, up_far = rows_of(gate_w, (opposite,)), rows_of(up_w, (opposite,))
    down_far, down_near = cols_of(down_w, (opposite,)), cols_of(down_w, (mate_a, mate_b, me))

    tables = []
    for first in range(0, capacity, SLOTS):
        slots = first + jnp.arange(SLOTS, dtype=jnp.int32)
        chosen = rank[:, None, :] == slots[None, :, None]
        rows = groups * SLOTS
        tables.append(
            [jnp.where(chosen, p[:, None, :], 0.0).reshape(rows, tok_count).astype(bf16) for p in (weight_high, weight_low)]
        )

    slots = jnp.arange(SLOTS, capacity, dtype=jnp.int32)
    chosen = (rank[:, None, :] == slots[None, :, None]).reshape(groups * (capacity - SLOTS), tok_count)
    sends = [first_send, dot(chosen.astype(bf16), normed).astype(bf16)]

    combined = jnp.zeros((tok_count, quarter), jnp.float32)
    for chunk, first in enumerate(range(0, capacity, SLOTS)):

        def exchange(x):
            return lax.all_to_all(x, "ep", split_axis=0, concat_axis=0, tiled=True)

        def shift(x, name):
            return lax.ppermute(x, "tp", even if name[1] == "r" else odd)

        half = rows // 2
        if chunk == 0:
            own = exchange(sends[0].reshape(groups, SLOTS, quarter)).reshape(rows, quarter)
            own, sends, tables, gate_near, up_near, gate_far, up_far, down_far, down_near = lax.optimization_barrier(
                (own, sends, tables, gate_near, up_near, gate_far, up_far, down_far, down_near)
            )
        elif chunk == 1:
            rest = exchange(sends[1].reshape(groups, capacity - SLOTS, quarter))
        if chunk:
            own = rest[:, first - SLOTS : first].reshape(rows, quarter)
        near_a = shift(own, "nr")
        near_b = shift(own, "nl")
        far_a = shift(near_b[:half], "fr")
        far_b = shift(near_a[half:], "fl")
        gate_sum, up_sum = first_call(own, near_a, near_b, gate_near, up_near)
        sent_a, sent_b, rest_a, rest_b, kept = last_call(
            gate_sum, up_sum, far_a, far_b, gate_far, up_far, down_far, down_near
        )
        f32 = jnp.float32
        got_a = shift(sent_a, "ar")
        got_b = shift(sent_b, "al")
        late_a = shift((rest_a.astype(f32) + got_b[:half].astype(f32)).astype(bf16), "br")
        late_b = shift((rest_b.astype(f32) + got_a[:half].astype(f32)).astype(bf16), "bl")
        result = total_call(kept, got_a, got_b, late_a, late_b).reshape(groups, SLOTS, quarter)
        returned = exchange(result).reshape(rows, quarter)
        table_high, table_low = tables[chunk]
        added = lax.dot_general(table_high, returned, (((0,), (0,)), ((), ())), preferred_element_type=jnp.float32)
        combined = combined + added
        added = lax.dot_general(table_low, returned, (((0,), (0,)), ((), ())), preferred_element_type=jnp.float32)
        combined = combined + added
        if first + SLOTS < capacity:
            combined = lax.optimization_barrier(combined)
    return combined.astype(bf16)


def solution(mesh):
    return jax.shard_map(
        layer,
        mesh=mesh,
        in_specs=(
            P("ep", None),
            P("ep", None),
            P("ep", None),
            P(),
            P("ep", None, "tp"),
            P("ep", None, "tp"),
            P("ep", "tp", None),
        ),
        out_specs=P("ep", "tp"),
        check_vma=False,
    )
```
